32 devices in a mesh: ep: 8 (over z, core), tp: 4 (over y, x).
Axes of the slice: x: 2, y: 2, z: 4, core: 2. Of those that a mesh axis runs over, the one named last changes fastest.
Arguments:
- tokens: bfloat16 [1024, 2048], P('ep'), may hold values from -6 to 6
- cotangent: bfloat16 [1024, 2048], P('ep'), may hold values from -6 to 6
- routes: int32 [1024, 2], P('ep'), may hold values from 0 to 7, all different within a row; in each aligned block of 128 rows (0 to 127, 128 to 255, ...) at most 64 rows name the same one
- route_weight: float32 [1024, 2], P('ep'), may hold values from 0.1 to 1
- w_gate: bfloat16 [8, 2048, 1024], P('ep', None, 'tp'), may hold values from -0.1875 to 0.1875
- w_up: bfloat16 [8, 2048, 1024], P('ep', None, 'tp'), may hold values from -0.1875 to 0.1875
- w_down: bfloat16 [8, 1024, 2048], P('ep', 'tp'), may hold values from -0.1875 to 0.1875
Outputs:
- grad_tokens: bfloat16 [1024, 2048], P('ep', 'tp')
- grad_route_weight: float32 [1024, 2], P('ep')
- grad_gate: float32 [8, 2048, 1024], P('ep', None, 'tp')
- grad_up: float32 [8, 2048, 1024], P('ep', None, 'tp')
- grad_down: float32 [8, 1024, 2048], P('ep', 'tp')
The draws below stay inside these ranges and needn't reach their ends.
Inputs may be any that keep to these rules, and one draw needn't show every extreme that they name: `routes`: each row names 2 different experts. In each aligned block of 128 rows (the rows of one index of ep) no expert is named by more than 64 rows, and in every draw some expert is named by exactly 64 rows of some block.
All inputs are finite; a program needn't handle non-finite values.
Results may differ from the reference program's by a relative error of at most 0.023.
Values may be sent and summed in bfloat16 or wider, within the bound.
A program may use at most 64 MiB of HBM per device.

```python
import math
import jax
import jax.numpy as jnp
import numpy as np
from jax import lax

D = 2048
FF = 1024
TOP_K = 2
TOK_DEV = 128
EXPERTS = 8
TOKENS = 1024
CAP = 64
N_EP = 8
N_TP = 4


def strengthened(result, rng, source, target, blocks, factor):
    def block_of(axis_at):
        return (jnp.arange(result.shape[axis_at]) // (result.shape[axis_at] // blocks)).reshape((-1,) + (1,) * (result.ndim - 1 - axis_at))

    near = jax.random.permutation(rng, blocks)[block_of(target)]
    second = (block_of(target) + blocks // 2) % blocks
    return jnp.where((block_of(source) == near) | (block_of(source) == second), factor * result, result)


def levels(rng, shape, cuts, least, top_value):
    def one(dim, shards_of):
        heights = jax.random.uniform(jax.random.fold_in(jax.random.fold_in(rng, 6), dim), (shards_of,), jnp.float32, least / len(cuts), top_value / len(cuts))
        return jnp.repeat(jnp.exp(heights), shape[dim] // shards_of).reshape((-1,) + (1,) * (len(shape) - dim - 1))

    gain = one(*cuts[0])
    for cut in cuts[1:]:
        gain = gain * one(*cut)
    return gain


def routed_block(own_key, own, number, rows, amount, top, bound, slope):
    ranking = jax.random.permutation(own_key, amount)
    packed, common = shares(amount, rows * top, bound, slope, True), shares(amount, rows * top, bound, slope, False)
    places = jnp.arange(amount)

    def named(lengths, rotation):
        used = int((lengths > 0).sum())
        fixed = max(1, used // 4)
        moved = fixed + (places - fixed + rotation * (used - fixed)) % max(1, amount - fixed)
        return jnp.zeros((amount,), jnp.int32).at[ranking[jnp.where(places < fixed, places, moved)]].set(jnp.asarray(lengths, jnp.int32))

    lengths = jnp.where(number % 4 == 0, named(packed, number // 4), named(common, number - number // 4 - 1))
    mixed = jax.random.permutation(jax.random.fold_in(own, 3), amount)
    giver, receiver = mixed[0:amount // 2 * 2:2], mixed[1:amount // 2 * 2:2]
    slack = jnp.minimum(lengths[giver] - 1, bound - lengths[receiver]) // 2
    slack = jnp.where((giver == ranking[0]) | (receiver == ranking[0]) | (lengths[receiver] == 0), 0, jnp.maximum(slack, 0))
    moved = jax.random.randint(jax.random.fold_in(own, 4), (amount // 2,), 0, 1 << 20) % (slack + 1)
    lengths = lengths.at[giver].add(-moved).at[receiver].add(moved)
    members = jnp.searchsorted(jnp.cumsum(lengths), jnp.arange(rows * top), side="right").astype(jnp.int32)
    grid = members.reshape(top, rows).T
    grid = grid[jax.random.permutation(jax.random.fold_in(own, 1), rows)]
    rotation = jax.random.randint(jax.random.fold_in(own, 2), (rows, 1), 0, top)
    return jnp.take_along_axis(grid, (jnp.arange(top)[None, :] + rotation) % top, axis=1)


def shares(number_of, total, bound, lean, full):
    portions = [(1 << 20) // math.isqrt(grade ** lean) + 1 for grade in range(1, number_of + 1)]
    largest = bound if full else min(bound, max(-(-total // number_of), total * portions[0] // sum(portions)))
    least = 1 if total - largest >= number_of - 1 else 0
    holding, surplus = [largest] + [least] * (number_of - 1), total - largest - least * (number_of - 1)
    while surplus > 0:
        free = [i for i in range(1, number_of) if holding[i] < largest] or [i for i in range(1, number_of) if holding[i] < bound]
        pool, budget = sum([portions[i] for i in free]), surplus
        for i in free:
            extra = min(bound - holding[i], max(1, budget * portions[i] // pool), surplus)
            holding[i] = holding[i] + extra
            surplus = surplus - extra
    return np.array(holding)


def scatter_about(stream_key, shape, scale, reach, cuts=(), kind=jnp.bfloat16):
    array = jax.random.normal(stream_key, shape, jnp.float32) * scale
    if len(cuts) > 0:
        array = levels(stream_key, shape, cuts, -0.22, 0.18) * array
    return jnp.clip(array, min=-reach, max=reach).astype(kind)


def gaussian_with(stream_key, shape, spread, reach, shards, heavy, held_as=jnp.bfloat16):
    entries = spread * jax.random.normal(stream_key, shape, jnp.float32)
    if shards:
        entries = entries * levels(stream_key, shape, shards, -0.22, 0.18)
    return jnp.clip(strengthened(entries, jax.random.fold_in(stream_key, 3), *heavy), -reach, reach).astype(held_as)


def setup_inputs(seed: int = 0) -> dict:
    key_list = jax.random.split(jax.random.key(seed), 8)
    tokens = scatter_about(key_list[0], (TOKENS, D), 1.0, 6.0, ((0, 8),))
    cotangent = scatter_about(key_list[1], (TOKENS, D), 1.0, 6.0, ((0, 8),))
    routes_keys = jax.random.split(jax.random.fold_in(key_list[2], 1), TOKENS // TOK_DEV)
    routes_turns = jax.random.permutation(jax.random.fold_in(key_list[2], 3), TOKENS // TOK_DEV)
    routes = jax.vmap(lambda own, number: routed_block(jax.random.fold_in(key_list[2], 2), own, number, TOK_DEV, EXPERTS, TOP_K, CAP, 2))(routes_keys, routes_turns).reshape((TOKENS, TOP_K))
    route_weight = jnp.clip(0.1 + 0.9 * jax.random.uniform(key_list[3], (TOKENS, TOP_K), jnp.float32) ** levels(key_list[3], (TOKENS, TOP_K), ((0, 8),), -0.2, 0.2), 0.1, 1.0)
    w_gate = gaussian_with(key_list[4], (EXPERTS, D, FF), D ** -0.5, 0.1875, ((0, 8), (2, 4)), (2, 1, 4, 2.0))
    w_up = gaussian_with(key_list[5], (EXPERTS, D, FF), D ** -0.5, 0.1875, ((0, 8), (2, 4)), (2, 1, 4, 2.0))
    w_down = scatter_about(key_list[6], (EXPERTS, FF, D), FF ** -0.5, 0.1875, ((0, 8), (1, 4)))
    return {"tokens": tokens, "cotangent": cotangent, "routes": routes, "route_weight": route_weight, "w_gate": w_gate, "w_up": w_up, "w_down": w_down}


def slot_index(block_routes, experts, capacity):
    flat_ids = block_routes.reshape(-1)
    onehot = (flat_ids[:, None] == jnp.arange(experts, dtype=jnp.int32)[None, :]).astype(jnp.int32)
    earlier = jnp.cumsum(onehot, axis=0) - onehot
    return flat_ids * capacity + jnp.sum(earlier * onehot, axis=1)


def expert_grads(inputs):
    rows_x, rows_dy, rows_w, gate_w, up_w, down_w = inputs
    f32 = jnp.float32
    n_rows, model_width = rows_x.shape
    gate_pre = jnp.dot(rows_x, gate_w, preferred_element_type=f32)
    up_pre = jnp.dot(rows_x, up_w, preferred_element_type=f32)
    gate_sig = jax.nn.sigmoid(gate_pre)
    act_full = gate_pre * gate_sig * up_pre
    act = act_full.astype(jnp.bfloat16)
    back_hidden = jnp.dot(rows_dy, down_w.T, preferred_element_type=f32)
    weighted_cot = (rows_w[:, None] * rows_dy.astype(f32)).astype(jnp.bfloat16)
    d_hidden = rows_w[:, None] * back_hidden
    d_gate = (d_hidden * up_pre * gate_sig * (1.0 + gate_pre * (1.0 - gate_sig))).astype(jnp.bfloat16)
    d_up = (d_hidden * gate_pre * gate_sig).astype(jnp.bfloat16)
    gate_grad = jnp.sum(act_full * back_hidden, axis=1)
    pieces = jnp.einsum('rjf,djf->jrd', d_gate.astype(f32).reshape(n_rows, N_TP, -1),
                        gate_w.astype(f32).reshape(model_width, N_TP, -1), precision=lax.Precision.HIGHEST)
    pieces = pieces + jnp.einsum('rjf,djf->jrd', d_up.astype(f32).reshape(n_rows, N_TP, -1),
                                 up_w.astype(f32).reshape(model_width, N_TP, -1), precision=lax.Precision.HIGHEST)
    rounded = lax.optimization_barrier(pieces.astype(jnp.bfloat16))
    route_grad = jnp.sum(rounded.astype(f32), axis=0).astype(jnp.bfloat16)
    grad_gate_e = jnp.dot(rows_x.T, d_gate, preferred_element_type=f32)
    grad_up_e = jnp.dot(rows_x.T, d_up, preferred_element_type=f32)
    grad_down_e = jnp.dot(act.T, weighted_cot, preferred_element_type=f32)
    return route_grad, gate_grad, grad_gate_e, grad_up_e, grad_down_e


def reference(tokens, cotangent, routes, route_weight, w_gate, w_up, w_down):
    f32 = jnp.float32
    blocks = routes.reshape(N_EP, TOK_DEV, TOP_K)
    slot_ids = jax.vmap(lambda block: slot_index(block, EXPERTS, CAP))(blocks)
    expert_ids = blocks.reshape(N_EP, TOK_DEV * TOP_K)
    positions = slot_ids - expert_ids * CAP
    sources = jnp.arange(N_EP, dtype=jnp.int32)[:, None]
    rows_x = jnp.repeat(tokens.reshape(N_EP, TOK_DEV, D), TOP_K, axis=1)
    rows_dy = jnp.repeat(cotangent.reshape(N_EP, TOK_DEV, D), TOP_K, axis=1)
    rows_w = route_weight.reshape(N_EP, TOK_DEV * TOP_K)
    buf_x = jnp.zeros((EXPERTS, N_EP, CAP, D), jnp.bfloat16).at[expert_ids, sources, positions].set(rows_x)
    buf_dy = jnp.zeros((EXPERTS, N_EP, CAP, D), jnp.bfloat16).at[expert_ids, sources, positions].set(rows_dy)
    buf_w = jnp.zeros((EXPERTS, N_EP, CAP), f32).at[expert_ids, sources, positions].set(rows_w)
    recv_rows = N_EP * CAP
    outs = lax.map(expert_grads, (buf_x.reshape(EXPERTS, recv_rows, D), buf_dy.reshape(EXPERTS, recv_rows, D),
                                  buf_w.reshape(EXPERTS, recv_rows), w_gate, w_up, w_down))
    route_grad, gate_grad, grad_gate, grad_up, grad_down = outs
    back_index = sources * CAP + positions
    picked = route_grad[expert_ids, back_index].astype(f32).reshape(TOKENS, TOP_K, D)
    grad_tokens = jnp.sum(picked, axis=1).astype(jnp.bfloat16)
    grad_route_weight = gate_grad[expert_ids, back_index].reshape(TOKENS, TOP_K)
    return grad_tokens, grad_route_weight, grad_gate, grad_up, grad_down
```

```python
import jax
import jax.numpy as jnp
from jax import lax
from jax.sharding import PartitionSpec as P


def slot_index(block_routes, experts, capacity):
    flat_ids = block_routes.reshape(-1)
    onehot = (flat_ids[:, None] == jnp.arange(experts, dtype=jnp.int32)[None, :]).astype(jnp.int32)
    earlier = jnp.cumsum(onehot, axis=0) - onehot
    return flat_ids * capacity + jnp.sum(earlier * onehot, axis=1)


def slotted(tokens, cotangent, routes, route_weight, w_gate, w_up, w_down):
    f32 = jnp.float32
    tok_rows, model_width = tokens.shape
    choices_row = routes.shape[1]
    experts = lax.axis_size("ep")
    capacity = 2 * tok_rows * choices_row // experts
    recv_rows = experts * capacity
    slot_ids = slot_index(routes, experts, capacity)
    send_w = jnp.zeros((recv_rows,), f32).at[slot_ids].set(route_weight.reshape(-1))
    send_x = (
        jnp.zeros((recv_rows, model_width), jnp.bfloat16)
        .at[slot_ids]
        .set(jnp.repeat(tokens, choices_row, axis=0))
    )
    send_dy = (
        jnp.zeros((recv_rows, model_width), jnp.bfloat16)
        .at[slot_ids]
        .set(jnp.repeat(cotangent, choices_row, axis=0))
    )
    got_x = lax.all_to_all(
        send_x.reshape(experts, capacity, model_width),
        "ep",
        split_axis=0,
        concat_axis=0,
        tiled=True,
    )
    got_dy, got_w = (
        lax.all_to_all(
            send_dy.reshape(experts, capacity, model_width),
            "ep",
            split_axis=0,
            concat_axis=0,
            tiled=True,
        ),
        lax.all_to_all(
            send_w.reshape(experts, capacity, 1).astype(jnp.bfloat16),
            "ep",
            split_axis=0,
            concat_axis=0,
            tiled=True,
        ).astype(jnp.float32),
    )
    rows_x = got_x.reshape(recv_rows, model_width)
    rows_dy = got_dy.reshape(recv_rows, model_width)
    rows_w = got_w.reshape(recv_rows)
    gate_w = w_gate[0]
    up_w = w_up[0]
    down_w = w_down[0]
    gate_pre = jnp.dot(rows_x, gate_w, preferred_element_type=f32)
    up_pre = jnp.dot(rows_x, up_w, preferred_element_type=f32)
    gate_sig = jax.nn.sigmoid(gate_pre)
    act_full = gate_pre * gate_sig * up_pre
    act = act_full.astype(jnp.bfloat16)
    back_hidden = jnp.einsum("rd,fd->rf", rows_dy, down_w, preferred_element_type=f32)
    weighted_cot = (rows_w[:, None] * rows_dy.astype(f32)).astype(jnp.bfloat16)
    d_hidden = rows_w[:, None] * back_hidden
    d_gate = (d_hidden * up_pre * gate_sig * (1.0 + gate_pre * (1.0 - gate_sig))).astype(
        jnp.bfloat16
    )
    d_up = (d_hidden * gate_pre * gate_sig).astype(jnp.bfloat16)
    gate_part = jnp.sum(act_full * back_hidden, axis=1)
    token_part = jnp.einsum("rf,df->rd", d_gate, gate_w, preferred_element_type=f32)
    token_part = token_part + jnp.einsum("rf,df->rd", d_up, up_w, preferred_element_type=f32)
    grad_gate = jnp.einsum("rd,rf->df", rows_x, d_gate, preferred_element_type=f32)[None]
    grad_up = jnp.einsum("rd,rf->df", rows_x, d_up, preferred_element_type=f32)[None]
    grad_down = jnp.einsum("rf,rd->fd", act, weighted_cot, preferred_element_type=f32)[None]
    rounded_part = token_part.astype(jnp.bfloat16).astype(f32)
    shares = lax.psum_scatter(
        rounded_part.astype(jnp.bfloat16), "tp", scatter_dimension=1, tiled=True
    )
    gate_total = lax.psum(gate_part, "tp")
    back_x, back_gate = (
        lax.all_to_all(
            shares.reshape(experts, capacity, -1), "ep", split_axis=0, concat_axis=0, tiled=True
        ),
        lax.all_to_all(
            gate_total.reshape(experts, capacity).astype(jnp.bfloat16),
            "ep",
            split_axis=0,
            concat_axis=0,
            tiled=True,
        ).astype(jnp.float32),
    )
    picked = back_x.reshape(recv_rows, -1)[slot_ids].astype(f32).reshape(tok_rows, choices_row, -1)
    grad_route_weight = back_gate.reshape(recv_rows)[slot_ids].reshape(tok_rows, choices_row)
    grad_tokens = jnp.sum(picked, axis=1).astype(jnp.bfloat16)
    return (grad_tokens, grad_route_weight, grad_gate, grad_up, grad_down)


def dense(tokens, cotangent, routes, route_weight, w_gate, w_up, w_down):
    f32, bf16 = jnp.float32, jnp.bfloat16
    rows, width = tokens.shape
    ep, tp = lax.axis_size("ep"), lax.axis_size("tp")
    cols = width // tp
    at = lax.axis_index("tp") * cols
    mine = jnp.stack([lax.dynamic_slice_in_dim(a, at, cols, 1) for a in (tokens, cotangent)])
    full = lax.all_gather(mine, ("ep", "tp"), tiled=False).reshape(ep, tp, 2, rows, cols)
    full = full.transpose(2, 0, 3, 1, 4).reshape(2, ep * rows, width)
    x, dy = full[0], full[1]
    hit = routes[None] == jnp.arange(ep, dtype=routes.dtype)[:, None, None]
    table = jnp.sum(jnp.where(hit, route_weight[None], 0.0), axis=2)
    w = lax.all_to_all(table, "ep", split_axis=0, concat_axis=0, tiled=True).reshape(-1)[:, None]
    g_w, u_w, d_w = w_gate[0], w_up[0], w_down[0]
    g = jnp.dot(x, g_w, preferred_element_type=f32)
    u = jnp.dot(x, u_w, preferred_element_type=f32)
    back = jnp.einsum("rd,fd->rf", dy, d_w, preferred_element_type=f32)
    sig = jax.nn.sigmoid(g)
    act = g * sig * u
    d_h = w * back
    d_gate = (d_h * u * sig * (1.0 + g * (1.0 - sig))).astype(bf16)
    d_up = (d_h * g * sig).astype(bf16)
    part = jnp.sum(act * back, axis=1)
    tok = jnp.einsum("rf,df->rd", d_gate, g_w, preferred_element_type=f32)
    tok = tok + jnp.einsum("rf,df->rd", d_up, u_w, preferred_element_type=f32)
    gg = jnp.einsum("rd,rf->df", x, d_gate, preferred_element_type=f32)[None]
    gu = jnp.einsum("rd,rf->df", x, d_up, preferred_element_type=f32)[None]
    gd = jnp.einsum("rf,rd->fd", (w * act).astype(bf16), dy, preferred_element_type=f32)[None]
    share = lax.psum_scatter(tok.astype(bf16), "tp", scatter_dimension=1, tiled=True)
    grad_tokens = lax.psum_scatter(share, "ep", scatter_dimension=0, tiled=True)
    total = lax.psum(part, "tp").reshape(ep, rows)
    home = lax.all_to_all(total, "ep", split_axis=0, concat_axis=0, tiled=True)
    grw = jnp.sum(jnp.where(hit, home[:, :, None], 0.0), axis=0)
    return grad_tokens, grw, gg, gu, gd


def on_device(*args):
    rows, width = args[0].shape
    gathered = 4 * rows * width * lax.axis_size("ep")
    return (dense if gathered <= 1 << 24 else slotted)(*args)


def solution(mesh):
    return jax.shard_map(
        on_device,
        mesh=mesh,
        in_specs=(
            P("ep", None),
            P("ep", None),
            P("ep", None),
            P("ep", None),
            P("ep", None, "tp"),
            P("ep", None, "tp"),
            P("ep", "tp", None),
        ),
        out_specs=(
            P("ep", "tp"),
            P("ep", None),
            P("ep", None, "tp"),
            P("ep", None, "tp"),
            P("ep", "tp", None),
        ),
        check_vma=False,
    )
```

```python
import functools

import jax
import jax.numpy as jnp
from jax import lax
from jax.experimental import pallas as pl
from jax.experimental.pallas import tpu as pltpu
from jax.sharding import PartitionSpec as P


def slot_index(block_routes, experts, capacity):
    flat_ids = block_routes.reshape(-1)
    onehot = (flat_ids[:, None] == jnp.arange(experts, dtype=jnp.int32)[None, :]).astype(jnp.int32)
    earlier = jnp.cumsum(onehot, axis=0) - onehot
    return flat_ids * capacity + jnp.sum(earlier * onehot, axis=1)


def slotted(tokens, cotangent, routes, route_weight, w_gate, w_up, w_down):
    f32 = jnp.float32
    tok_rows, model_width = tokens.shape
    choices_row = routes.shape[1]
    experts = lax.axis_size("ep")
    capacity = 2 * tok_rows * choices_row // experts
    recv_rows = experts * capacity
    slot_ids = slot_index(routes, experts, capacity)
    send_w = jnp.zeros((recv_rows,), f32).at[slot_ids].set(route_weight.reshape(-1))
    send_x = (
        jnp.zeros((recv_rows, model_width), jnp.bfloat16)
        .at[slot_ids]
        .set(jnp.repeat(tokens, choices_row, axis=0))
    )
    send_dy = (
        jnp.zeros((recv_rows, model_width), jnp.bfloat16)
        .at[slot_ids]
        .set(jnp.repeat(cotangent, choices_row, axis=0))
    )
    got_x = lax.all_to_all(
        send_x.reshape(experts, capacity, model_width),
        "ep",
        split_axis=0,
        concat_axis=0,
        tiled=True,
    )
    got_dy, got_w = (
        lax.all_to_all(
            send_dy.reshape(experts, capacity, model_width),
            "ep",
            split_axis=0,
            concat_axis=0,
            tiled=True,
        ),
        lax.all_to_all(
            send_w.reshape(experts, capacity, 1).astype(jnp.bfloat16),
            "ep",
            split_axis=0,
            concat_axis=0,
            tiled=True,
        ).astype(jnp.float32),
    )
    rows_x = got_x.reshape(recv_rows, model_width)
    rows_dy = got_dy.reshape(recv_rows, model_width)
    rows_w = got_w.reshape(recv_rows)
    gate_w = w_gate[0]
    up_w = w_up[0]
    down_w = w_down[0]
    gate_pre = jnp.dot(rows_x, gate_w, preferred_element_type=f32)
    up_pre = jnp.dot(rows_x, up_w, preferred_element_type=f32)
    gate_sig = jax.nn.sigmoid(gate_pre)
    act_full = gate_pre * gate_sig * up_pre
    act = act_full.astype(jnp.bfloat16)
    back_hidden = jnp.einsum("rd,fd->rf", rows_dy, down_w, preferred_element_type=f32)
    weighted_cot = (rows_w[:, None] * rows_dy.astype(f32)).astype(jnp.bfloat16)
    d_hidden = rows_w[:, None] * back_hidden
    d_gate = (d_hidden * up_pre * gate_sig * (1.0 + gate_pre * (1.0 - gate_sig))).astype(
        jnp.bfloat16
    )
    d_up = (d_hidden * gate_pre * gate_sig).astype(jnp.bfloat16)
    gate_part = jnp.sum(act_full * back_hidden, axis=1)
    token_part = jnp.einsum("rf,df->rd", d_gate, gate_w, preferred_element_type=f32)
    token_part = token_part + jnp.einsum("rf,df->rd", d_up, up_w, preferred_element_type=f32)
    grad_gate = jnp.einsum("rd,rf->df", rows_x, d_gate, preferred_element_type=f32)[None]
    grad_up = jnp.einsum("rd,rf->df", rows_x, d_up, preferred_element_type=f32)[None]
    grad_down = jnp.einsum("rf,rd->fd", act, weighted_cot, preferred_element_type=f32)[None]
    rounded_part = token_part.astype(jnp.bfloat16).astype(f32)
    shares = lax.psum_scatter(
        rounded_part.astype(jnp.bfloat16), "tp", scatter_dimension=1, tiled=True
    )
    gate_total = lax.psum(gate_part, "tp")
    back_x, back_gate = (
        lax.all_to_all(
            shares.reshape(experts, capacity, -1), "ep", split_axis=0, concat_axis=0, tiled=True
        ),
        lax.all_to_all(
            gate_total.reshape(experts, capacity).astype(jnp.bfloat16),
            "ep",
            split_axis=0,
            concat_axis=0,
            tiled=True,
        ).astype(jnp.float32),
    )
    picked = back_x.reshape(recv_rows, -1)[slot_ids].astype(f32).reshape(tok_rows, choices_row, -1)
    grad_route_weight = back_gate.reshape(recv_rows)[slot_ids].reshape(tok_rows, choices_row)
    grad_tokens = jnp.sum(picked, axis=1).astype(jnp.bfloat16)
    return (grad_tokens, grad_route_weight, grad_gate, grad_up, grad_down)


def kernel(ep, tp, tokens, cotangent, table, w_gate, w_up, w_down,
           out_tok, out_home, out_gate, out_up, out_down,
           full, gate_v, up_v, down_v, weights, part, other, top, bottom,
           in_top, in_bottom, last_top, last_bottom, share, arrived,
           d_gate, d_up, act_w, g_gate, g_up, g_down, score, scores, total, home, result,
           local, sent, got):
    f32, bf16 = jnp.float32, jnp.bfloat16
    rows, width = tokens.shape
    cols = width // tp
    half = rows // 2
    nz = ep // 2
    e, t = lax.axis_index("ep"), lax.axis_index("tp")
    z, c = e // 2, lax.rem(e, 2)
    y, x = t // 2, lax.rem(t, 2)
    side = z * 2 + 1 - c
    tx, ty = y * 2 + 1 - x, (1 - y) * 2 + x
    td = (1 - y) * 2 + 1 - x
    slots, started, locals_ = {}, [], []

    def slot(*name):
        return got.at[slots.setdefault(name, len(slots))]

    def push(src, dst, name, to_e, to_t):
        copy = pltpu.make_async_remote_copy(
            src_ref=src, dst_ref=dst, send_sem=sent.at[len(started)], recv_sem=slot(*name),
            device_id={"ep": to_e, "tp": to_t}, device_id_type=pl.DeviceIdType.MESH)
        copy.start()
        started.append(copy)

    def landed(dst, *name):
        pltpu.make_async_remote_copy(
            src_ref=dst, dst_ref=dst, send_sem=sent.at[0], recv_sem=slot(*name),
            device_id={"ep": side, "tp": t}, device_id_type=pl.DeviceIdType.MESH).wait_recv()

    def bring(src, dst):
        copy = pltpu.make_async_copy(src, dst, local.at[len(locals_)])
        copy.start()
        locals_.append(copy)
        return copy

    own = [bring(ref.at[:, pl.ds(q * cols, cols)], full.at[e, a, q])
           for a, ref in enumerate((tokens, cotangent)) for q in range(tp)]
    loads = [bring(w_gate.at[0], gate_v), bring(w_up.at[0], up_v), bring(w_down.at[0], down_v)]
    weights[e] = table[...]

    barrier = pltpu.get_barrier_semaphore()
    for k in range(1, ep):
        pl.semaphore_signal(barrier, inc=1, device_id={"ep": lax.rem(e + k, ep), "tp": t},
                            device_id_type=pl.DeviceIdType.MESH)
    for k in range(1, tp):
        pl.semaphore_signal(barrier, inc=1, device_id={"ep": e, "tp": lax.rem(t + k, tp)},
                            device_id_type=pl.DeviceIdType.MESH)
    pl.semaphore_wait(barrier, ep + tp - 2)

    def back(dz):
        return lax.rem(z - dz + nz, nz)

    for copy in own:
        copy.wait()
    for dz in range(1, nz):
        for a in range(2):
            push(full.at[e, a, t], full.at[e, a, t], ("z", dz, a), lax.rem(z + dz, nz) * 2 + c, t)
    for a in range(2):
        push(full.at[e, a], full.at[e, a], ("side", 0, a), side, t)
    for k in range(1, ep):
        push(table, weights.at[e], ("w", k), lax.rem(e + k, ep), t)

    def spread(dz):
        s = back(dz) * 2 + c
        for a in range(2):
            piece = full.at[s, a, t]
            landed(piece, "z", dz, a)
            push(piece, piece, ("x", dz, a), e, tx)
            push(piece, piece, ("y", dz, a), e, ty)

    def relay(dz):
        s = back(dz) * 2 + c
        piece = full.at[s, 0, ty]
        landed(piece, "y", dz, 0)
        push(piece, piece, ("d", dz, 0), e, tx)
        piece = full.at[s, 1, tx]
        landed(piece, "x", dz, 1)
        push(piece, piece, ("d", dz, 1), e, ty)

    def hand(dz):
        s = back(dz) * 2 + c
        landed(full.at[s, 0, tx], "x", dz, 0)
        landed(full.at[s, 0, td], "d", dz, 0)
        push(full.at[s, 0], full.at[s, 0], ("side", dz, 0), side, t)
        landed(full.at[s, 1, ty], "y", dz, 1)
        landed(full.at[s, 1, td], "d", dz, 1)
        push(full.at[s, 1], full.at[s, 1], ("side", dz, 1), side, t)

    def nt(a, b):
        return lax.dot_general(a, b, (((1,), (1,)), ((), ())), preferred_element_type=f32)

    def tn(a, b):
        return lax.dot_general(a, b, (((0,), (0,)), ((), ())), preferred_element_type=f32)

    def column(block):
        mine = lax.broadcasted_iota(jnp.int32, (ep, rows), 0) == e
        row = jnp.sum(jnp.where(mine, weights[block], 0.0), axis=0, keepdims=True)
        return jnp.transpose(jnp.broadcast_to(row, (rows, rows)))[:, :1]

    def compute(dz):
        b = back(dz) * 2
        for a in range(2):
            landed(full.at[back(dz) * 2 + 1 - c, a], "side", dz, a)
        g = u = bk = None
        for q in range(tp):
            span = pl.ds(q * cols, cols)
            xs = jnp.concatenate([full[b, 0, q], full[b + 1, 0, q]], axis=0)
            dy = jnp.concatenate([full[b, 1, q], full[b + 1, 1, q]], axis=0)
            g_q = jnp.dot(xs, gate_v[span, :], preferred_element_type=f32)
            u_q = jnp.dot(xs, up_v[span, :], preferred_element_type=f32)
            b_q = nt(dy, down_v[:, span])
            g, u, bk = (g_q, u_q, b_q) if q == 0 else (g + g_q, u + u_q, bk + b_q)
        w = jnp.concatenate([column(b), column(b + 1)], axis=0)
        sig = jax.nn.sigmoid(g)
        silu = g * sig
        act = silu * u
        d_h = w * bk
        dg = (d_h * u * sig * (1.0 + g * (1.0 - sig))).astype(bf16)
        du = (d_h * silu).astype(bf16)
        aw = (w * act).astype(bf16)
        sums = jnp.sum(act * bk, axis=1, keepdims=True)
        for i in range(2):
            cut = slice(i * rows, (i + 1) * rows)
            d_gate[b + i] = dg[cut]
            d_up[b + i] = du[cut]
            act_w[b + i] = aw[cut]
            score[b + i] = jnp.transpose(jnp.broadcast_to(sums[cut], (rows, rows)))[:8]
        for q in range(tp):
            span = pl.ds(q * cols, cols)
            piece = (nt(dg, gate_v[span, :]) + nt(du, up_v[span, :])).astype(bf16)
            part[b, q] = piece[:rows]
            part[b + 1, q] = piece[rows:]
        push(part.at[back(dz) * 2 + 1 - c], other.at[dz], ("pair", dz), side, t)

    for copy in loads:
        copy.wait()
    for k in range(1, ep):
        landed(weights.at[lax.rem(e - k + ep, ep)], "w", k)
    spread(1)
    compute(0)
    for dz in range(1, nz):
        relay(dz)
        if dz + 1 < nz:
            spread(dz + 1)
        hand(dz)
        compute(dz)

    for k in range(1, tp):
        push(score, scores.at[t], ("score", k), e, lax.rem(t + k, tp))
    order = list(range(1, nz)) + [0]

    def add(*terms):
        value = terms[0].astype(f32)
        for term in terms[1:]:
            value = value + term.astype(f32)
        return value

    def first(dz):
        s = back(dz) * 2 + c
        landed(other.at[dz], "pair", dz)
        for r, q in enumerate((t, ty, tx, td)):
            top[dz, r] = add(part[s, q, :half], other[dz, q, :half]).astype(bf16)
        push(top.at[dz, pl.ds(2, 2)], in_top.at[dz], ("top", dz), e, tx)
        for r, q in enumerate((t, tx, ty, td)):
            bottom[dz, r] = add(part[s, q, half:], other[dz, q, half:]).astype(bf16)
        push(bottom.at[dz, pl.ds(2, 2)], in_bottom.at[dz], ("bottom", dz), e, ty)

    def second(dz):
        landed(in_top.at[dz], "top", dz)
        top[dz, 1] = add(top[dz, 1], in_top[dz, 1]).astype(bf16)
        push(top.at[dz, 1], last_top.at[dz], ("last_top", dz), e, ty)
        landed(in_bottom.at[dz], "bottom", dz)
        bottom[dz, 1] = add(bottom[dz, 1], in_bottom[dz, 1]).astype(bf16)
        push(bottom.at[dz, 1], last_bottom.at[dz], ("last_bottom", dz), e, tx)

    def third(dz):
        landed(last_top.at[dz], "last_top", dz)
        landed(last_bottom.at[dz], "last_bottom", dz)
        upper = add(top[dz, 0], in_top[dz, 0], last_top[dz])
        lower = add(bottom[dz, 0], in_bottom[dz, 0], last_bottom[dz])
        if dz:
            share[dz - 1, :half] = upper.astype(bf16)
            share[dz - 1, half:] = lower.astype(bf16)
            push(share.at[dz - 1], arrived.at[dz - 1], ("share", dz), back(dz) * 2 + c, t)
        return upper, lower

    def by_width(out, ref, dst):
        right = ref[...].reshape(ep * rows, ref.shape[2])
        for q in range(tp):
            out[pl.ds(q * cols, cols), :] = tn(full[:, 0, q].reshape(ep * rows, cols), right)
        bring(out, dst.at[0])

    for dz in order:
        first(dz)
    by_width(g_gate, d_gate, out_gate)
    second(order[0])
    second(order[1])
    by_width(g_up, d_up, out_up)
    scores[t] = score[...]
    for k in range(1, tp):
        landed(scores.at[lax.rem(t - k + tp, tp)], "score", k)
    total[...] = add(*[scores[j] for j in range(tp)])
    for k in range(1, ep):
        to = lax.rem(e + k, ep)
        push(total.at[to], home.at[e], ("home", k), to, t)
    home[e] = total[e]
    for dz in order[2:]:
        second(dz)
    for dz in order[:-1]:
        third(dz)
    left = act_w[...].reshape(ep * rows, act_w.shape[2])
    for q in range(tp):
        g_down[:, pl.ds(q * cols, cols)] = tn(left, full[:, 1, q].reshape(ep * rows, cols))
    bring(g_down, out_down.at[0])
    upper, lower = third(0)
    for dz in range(1, nz):
        landed(arrived.at[dz - 1], "share", dz)
        upper = upper + arrived[dz - 1, :half].astype(f32)
        lower = lower + arrived[dz - 1, half:].astype(f32)
    result[:half] = upper.astype(bf16)
    result[half:] = lower.astype(bf16)
    bring(result, out_tok)
    for k in range(1, ep):
        landed(home.at[lax.rem(e - k + ep, ep)], "home", k)
    for j in range(ep):
        out_home[pl.ds(j, 1), :] = home[j, :1]
    for copy in started:
        copy.wait_send()
    for copy in locals_[len(own) + len(loads):]:
        copy.wait()


def dense(tokens, cotangent, routes, route_weight, w_gate, w_up, w_down):
    f32, bf16 = jnp.float32, jnp.bfloat16
    rows, width = tokens.shape
    ep, tp = lax.axis_size("ep"), lax.axis_size("tp")
    cols, half, nz, hidden = width // tp, rows // 2, ep // 2, w_gate.shape[2]
    hit = routes[None] == jnp.arange(ep, dtype=routes.dtype)[:, None, None]
    table = jnp.sum(jnp.where(hit, route_weight[None], 0.0), axis=2)
    anywhere, near = pl.BlockSpec(memory_space=pl.ANY), pl.BlockSpec(memory_space=pltpu.VMEM)
    shape = jax.ShapeDtypeStruct
    grad_tokens, home, gg, gu, gd = pl.pallas_call(
        functools.partial(kernel, ep, tp),
        out_shape=(shape((rows, cols), bf16), shape((ep, rows), f32), shape(w_gate.shape, f32),
                   shape(w_up.shape, f32), shape(w_down.shape, f32)),
        in_specs=[anywhere, anywhere, near, anywhere, anywhere, anywhere],
        out_specs=(anywhere, near, anywhere, anywhere, anywhere),
        scratch_shapes=[
            pltpu.VMEM((ep, 2, tp, rows, cols), bf16),
            pltpu.VMEM((width, hidden), bf16),
            pltpu.VMEM((width, hidden), bf16),
            pltpu.VMEM((hidden, width), bf16),
            pltpu.VMEM((ep, ep, rows), f32),
            pltpu.VMEM((ep, tp, rows, cols), bf16),
            pltpu.VMEM((nz, tp, rows, cols), bf16),
            pltpu.VMEM((nz, 4, half, cols), bf16),
            pltpu.VMEM((nz, 4, half, cols), bf16),
            pltpu.VMEM((nz, 2, half, cols), bf16),
            pltpu.VMEM((nz, 2, half, cols), bf16),
            pltpu.VMEM((nz, half, cols), bf16),
            pltpu.VMEM((nz, half, cols), bf16),
            pltpu.VMEM((nz - 1, rows, cols), bf16),
            pltpu.VMEM((nz - 1, rows, cols), bf16),
            pltpu.VMEM((ep, rows, hidden), bf16),
            pltpu.VMEM((ep, rows, hidden), bf16),
            pltpu.VMEM((ep, rows, hidden), bf16),
            pltpu.VMEM((width, hidden), f32),
            pltpu.VMEM((width, hidden), f32),
            pltpu.VMEM((hidden, width), f32),
            pltpu.VMEM((ep, 8, rows), f32),
            pltpu.VMEM((tp, ep, 8, rows), f32),
            pltpu.VMEM((ep, 8, rows), f32),
            pltpu.VMEM((ep, 8, rows), f32),
            pltpu.VMEM((rows, cols), bf16),
            pltpu.SemaphoreType.DMA((16 + 2 * tp,)),
            pltpu.SemaphoreType.DMA((24 * nz,)),
            pltpu.SemaphoreType.DMA((24 * nz,)),
        ],
        compiler_params=pltpu.CompilerParams(
            collective_id=0, has_side_effects=True, vmem_limit_bytes=50 * 1024 * 1024),
    )(tokens, cotangent, table, w_gate, w_up, w_down)
    grw = jnp.sum(jnp.where(hit, home[:, :, None], 0.0), axis=0)
    return grad_tokens, grw, gg, gu, gd


def on_device(*args):
    rows, width = args[0].shape
    ep, tp = lax.axis_size("ep"), lax.axis_size("tp")
    fits = tp == 4 and ep % 2 == 0 and rows % 128 == 0 and 4 * rows * width * ep <= 1 << 24
    return (dense if fits else slotted)(*args)


def solution(mesh):
    return jax.shard_map(
        on_device,
        mesh=mesh,
        in_specs=(
            P("ep", None),
            P("ep", None),
            P("ep", None),
            P("ep", None),
            P("ep", None, "tp"),
            P("ep", None, "tp"),
            P("ep", "tp", None),
        ),
        out_specs=(
            P("ep", "tp"),
            P("ep", None),
            P("ep", None, "tp"),
            P("ep", None, "tp"),
            P("ep", "tp", None),
        ),
        check_vma=False,
    )
```

```python
import functools

import jax
import jax.numpy as jnp
from jax import lax
from jax.experimental import pallas as pl
from jax.experimental.pallas import tpu as pltpu
from jax.sharding import PartitionSpec as P


def slot_index(block_routes, experts, capacity):
    flat_ids = block_routes.reshape(-1)
    onehot = (flat_ids[:, None] == jnp.arange(experts, dtype=jnp.int32)[None, :]).astype(jnp.int32)
    earlier = jnp.cumsum(onehot, axis=0) - onehot
    return flat_ids * capacity + jnp.sum(earlier * onehot, axis=1)


def slotted(tokens, cotangent, routes, route_weight, w_gate, w_up, w_down):
    f32 = jnp.float32
    tok_rows, model_width = tokens.shape
    choices_row = routes.shape[1]
    experts = lax.axis_size("ep")
    capacity = 2 * tok_rows * choices_row // experts
    recv_rows = experts * capacity
    slot_ids = slot_index(routes, experts, capacity)
    send_w = jnp.zeros((recv_rows,), f32).at[slot_ids].set(route_weight.reshape(-1))
    send_x = (
        jnp.zeros((recv_rows, model_width), jnp.bfloat16)
        .at[slot_ids]
        .set(jnp.repeat(tokens, choices_row, axis=0))
    )
    send_dy = (
        jnp.zeros((recv_rows, model_width), jnp.bfloat16)
        .at[slot_ids]
        .set(jnp.repeat(cotangent, choices_row, axis=0))
    )
    got_x = lax.all_to_all(
        send_x.reshape(experts, capacity, model_width),
        "ep",
        split_axis=0,
        concat_axis=0,
        tiled=True,
    )
    got_dy, got_w = (
        lax.all_to_all(
            send_dy.reshape(experts, capacity, model_width),
            "ep",
            split_axis=0,
            concat_axis=0,
            tiled=True,
        ),
        lax.all_to_all(
            send_w.reshape(experts, capacity, 1).astype(jnp.bfloat16),
            "ep",
            split_axis=0,
            concat_axis=0,
            tiled=True,
        ).astype(jnp.float32),
    )
    rows_x = got_x.reshape(recv_rows, model_width)
    rows_dy = got_dy.reshape(recv_rows, model_width)
    rows_w = got_w.reshape(recv_rows)
    gate_w = w_gate[0]
    up_w = w_up[0]
    down_w = w_down[0]
    gate_pre = jnp.dot(rows_x, gate_w, preferred_element_type=f32)
    up_pre = jnp.dot(rows_x, up_w, preferred_element_type=f32)
    gate_sig = jax.nn.sigmoid(gate_pre)
    act_full = gate_pre * gate_sig * up_pre
    act = act_full.astype(jnp.bfloat16)
    back_hidden = jnp.einsum("rd,fd->rf", rows_dy, down_w, preferred_element_type=f32)
    weighted_cot = (rows_w[:, None] * rows_dy.astype(f32)).astype(jnp.bfloat16)
    d_hidden = rows_w[:, None] * back_hidden
    d_gate = (d_hidden * up_pre * gate_sig * (1.0 + gate_pre * (1.0 - gate_sig))).astype(
        jnp.bfloat16
    )
    d_up = (d_hidden * gate_pre * gate_sig).astype(jnp.bfloat16)
    gate_part = jnp.sum(act_full * back_hidden, axis=1)
    token_part = jnp.einsum("rf,df->rd", d_gate, gate_w, preferred_element_type=f32)
    token_part = token_part + jnp.einsum("rf,df->rd", d_up, up_w, preferred_element_type=f32)
    grad_gate = jnp.einsum("rd,rf->df", rows_x, d_gate, preferred_element_type=f32)[None]
    grad_up = jnp.einsum("rd,rf->df", rows_x, d_up, preferred_element_type=f32)[None]
    grad_down = jnp.einsum("rf,rd->fd", act, weighted_cot, preferred_element_type=f32)[None]
    rounded_part = token_part.astype(jnp.bfloat16).astype(f32)
    shares = lax.psum_scatter(
        rounded_part.astype(jnp.bfloat16), "tp", scatter_dimension=1, tiled=True
    )
    gate_total = lax.psum(gate_part, "tp")
    back_x, back_gate = (
        lax.all_to_all(
            shares.reshape(experts, capacity, -1), "ep", split_axis=0, concat_axis=0, tiled=True
        ),
        lax.all_to_all(
            gate_total.reshape(experts, capacity).astype(jnp.bfloat16),
            "ep",
            split_axis=0,
            concat_axis=0,
            tiled=True,
        ).astype(jnp.float32),
    )
    picked = back_x.reshape(recv_rows, -1)[slot_ids].astype(f32).reshape(tok_rows, choices_row, -1)
    grad_route_weight = back_gate.reshape(recv_rows)[slot_ids].reshape(tok_rows, choices_row)
    grad_tokens = jnp.sum(picked, axis=1).astype(jnp.bfloat16)
    return (grad_tokens, grad_route_weight, grad_gate, grad_up, grad_down)


def kernel(ep, tp, tokens, cotangent, table, w_gate, w_up, w_down,
           out_tok, out_home, out_gate, out_up, out_down,
           full, gate_v, up_v, down_v, weights, part, other, top, bottom,
           in_top, in_bottom, last_top, last_bottom, share, arrived,
           d_gate, d_up, act_w, g_gate, g_up, g_down, score, scores, total, home, result,
           local, sent, got):
    f32, bf16 = jnp.float32, jnp.bfloat16
    rows, width = tokens.shape
    cols = width // tp
    half = rows // 2
    nz = ep // 2
    e, t = lax.axis_index("ep"), lax.axis_index("tp")
    z, c = e // 2, lax.rem(e, 2)
    y, x = t // 2, lax.rem(t, 2)
    side = z * 2 + 1 - c
    tx, ty = y * 2 + 1 - x, (1 - y) * 2 + x
    td = (1 - y) * 2 + 1 - x
    slots, started, locals_ = {}, [], []

    def slot(*name):
        return got.at[slots.setdefault(name, len(slots))]

    def push(src, dst, name, to_e, to_t):
        copy = pltpu.make_async_remote_copy(
            src_ref=src, dst_ref=dst, send_sem=sent.at[len(started)], recv_sem=slot(*name),
            device_id={"ep": to_e, "tp": to_t}, device_id_type=pl.DeviceIdType.MESH)
        copy.start()
        started.append(copy)

    def landed(dst, *name):
        pltpu.make_async_remote_copy(
            src_ref=dst, dst_ref=dst, send_sem=sent.at[0], recv_sem=slot(*name),
            device_id={"ep": side, "tp": t}, device_id_type=pl.DeviceIdType.MESH).wait_recv()

    def bring(src, dst):
        copy = pltpu.make_async_copy(src, dst, local.at[len(locals_)])
        copy.start()
        locals_.append(copy)
        return copy

    own = [bring(ref.at[:, pl.ds(q * cols, cols)], full.at[e, a, q])
           for a, ref in enumerate((tokens, cotangent)) for q in range(tp)]
    loads = [bring(w_gate.at[0], gate_v), bring(w_up.at[0], up_v), bring(w_down.at[0], down_v)]
    weights[e] = table[...]

    barrier = pltpu.get_barrier_semaphore()
    for k in range(1, ep):
        pl.semaphore_signal(barrier, inc=1, device_id={"ep": lax.rem(e + k, ep), "tp": t},
                            device_id_type=pl.DeviceIdType.MESH)
    for k in range(1, tp):
        pl.semaphore_signal(barrier, inc=1, device_id={"ep": e, "tp": lax.rem(t + k, tp)},
                            device_id_type=pl.DeviceIdType.MESH)
    pl.semaphore_wait(barrier, ep + tp - 2)

    edge = jnp.minimum(z, nz - 1 - z)

    def back(i):
        near = z + (i + 1) // 2 * (1 - i % 2 * 2)
        away = jnp.where(z < nz - 1 - z, z + i - edge, z - i + edge)
        return jnp.where(i <= 2 * edge, near, away) if i else z

    relays = []

    def along(piece, from_z, a, go, to_z):
        copy = pltpu.make_async_remote_copy(
            src_ref=piece, dst_ref=piece, send_sem=sent.at[20 * nz + len(relays)],
            recv_sem=got.at[20 * nz + from_z * 2 + a],
            device_id={"ep": to_z * 2 + c, "tp": t}, device_id_type=pl.DeviceIdType.MESH)
        pl.when(go)(copy.start)
        relays.append((go, copy))

    for copy in own:
        copy.wait()
    for a in range(2):
        along(full.at[e, a, t], z, a, z < nz - 1, jnp.minimum(z + 1, nz - 1))
        along(full.at[e, a, t], z, a, z > 0, jnp.maximum(z - 1, 0))
    for a in range(2):
        push(full.at[e, a], full.at[e, a], ("side", 0, a), side, t)
    for k in range(1, ep):
        push(table, weights.at[e], ("w", k), lax.rem(e + k, ep), t)

    def spread(dz):
        s = back(dz) * 2 + c
        for a in range(2):
            piece = full.at[s, a, t]
            pltpu.make_async_remote_copy(
                src_ref=piece, dst_ref=piece, send_sem=sent.at[0],
                recv_sem=got.at[20 * nz + back(dz) * 2 + a],
                device_id={"ep": side, "tp": t}, device_id_type=pl.DeviceIdType.MESH).wait_recv()
            below = back(dz) < z
            go = jnp.where(below, z < nz - 1, z > 0)
            onward = jnp.where(below, jnp.minimum(z + 1, nz - 1), jnp.maximum(z - 1, 0))
            along(piece, back(dz), a, go, onward)
            push(piece, piece, ("x", dz, a), e, tx)
            push(piece, piece, ("y", dz, a), e, ty)

    def relay(dz):
        s = back(dz) * 2 + c
        piece = full.at[s, 0, ty]
        landed(piece, "y", dz, 0)
        push(piece, piece, ("d", dz, 0), e, tx)
        piece = full.at[s, 1, tx]
        landed(piece, "x", dz, 1)
        push(piece, piece, ("d", dz, 1), e, ty)

    def hand(dz):
        s = back(dz) * 2 + c
        landed(full.at[s, 0, tx], "x", dz, 0)
        landed(full.at[s, 0, td], "d", dz, 0)
        push(full.at[s, 0], full.at[s, 0], ("side", dz, 0), side, t)
        landed(full.at[s, 1, ty], "y", dz, 1)
        landed(full.at[s, 1, td], "d", dz, 1)
        push(full.at[s, 1], full.at[s, 1], ("side", dz, 1), side, t)

    def nt(a, b):
        return lax.dot_general(a, b, (((1,), (1,)), ((), ())), preferred_element_type=f32)

    def tn(a, b):
        return lax.dot_general(a, b, (((0,), (0,)), ((), ())), preferred_element_type=f32)

    def column(block):
        mine = lax.broadcasted_iota(jnp.int32, (ep, rows), 0) == e
        row = jnp.sum(jnp.where(mine, weights[block], 0.0), axis=0, keepdims=True)
        return jnp.transpose(jnp.broadcast_to(row, (rows, rows)))[:, :1]

    def compute(dz):
        b = back(dz) * 2
        for a in range(2):
            landed(full.at[back(dz) * 2 + 1 - c, a], "side", dz, a)
        g = u = bk = None
        for q in range(tp):
            span = pl.ds(q * cols, cols)
            xs = jnp.concatenate([full[b, 0, q], full[b + 1, 0, q]], axis=0)
            dy = jnp.concatenate([full[b, 1, q], full[b + 1, 1, q]], axis=0)
            g_q = jnp.dot(xs, gate_v[span, :], preferred_element_type=f32)
            u_q = jnp.dot(xs, up_v[span, :], preferred_element_type=f32)
            b_q = nt(dy, down_v[:, span])
            g, u, bk = (g_q, u_q, b_q) if q == 0 else (g + g_q, u + u_q, bk + b_q)
        w = jnp.concatenate([column(b), column(b + 1)], axis=0)
        sig = jax.nn.sigmoid(g)
        silu = g * sig
        act = silu * u
        d_h = w * bk
        dg = (d_h * u * sig * (1.0 + g * (1.0 - sig))).astype(bf16)
        du = (d_h * silu).astype(bf16)
        aw = (w * act).astype(bf16)
        sums = jnp.sum(act * bk, axis=1, keepdims=True)
        for i in range(2):
            cut = slice(i * rows, (i + 1) * rows)
            d_gate[b + i] = dg[cut]
            d_up[b + i] = du[cut]
            act_w[b + i] = aw[cut]
            score[b + i] = jnp.transpose(jnp.broadcast_to(sums[cut], (rows, rows)))[:8]
        for q in range(tp):
            span = pl.ds(q * cols, cols)
            piece = (nt(dg, gate_v[span, :]) + nt(du, up_v[span, :])).astype(bf16)
            part[b, q] = piece[:rows]
            part[b + 1, q] = piece[rows:]
        push(part.at[back(dz) * 2 + 1 - c], other.at[dz], ("pair", dz), side, t)

    for copy in loads:
        copy.wait()
    for k in range(1, ep):
        landed(weights.at[lax.rem(e - k + ep, ep)], "w", k)

    def add(*terms):
        value = terms[0].astype(f32)
        for term in terms[1:]:
            value = value + term.astype(f32)
        return value

    def first(dz):
        s = back(dz) * 2 + c
        landed(other.at[dz], "pair", dz)
        for r, q in enumerate((t, ty, tx, td)):
            top[dz, r] = add(part[s, q, :half], other[dz, q, :half]).astype(bf16)
        push(top.at[dz, pl.ds(2, 2)], in_top.at[dz], ("top", dz), e, tx)
        for r, q in enumerate((t, tx, ty, td)):
            bottom[dz, r] = add(part[s, q, half:], other[dz, q, half:]).astype(bf16)
        push(bottom.at[dz, pl.ds(2, 2)], in_bottom.at[dz], ("bottom", dz), e, ty)

    def second(dz):
        landed(in_top.at[dz], "top", dz)
        top[dz, 1] = add(top[dz, 1], in_top[dz, 1]).astype(bf16)
        push(top.at[dz, 1], last_top.at[dz], ("last_top", dz), e, ty)
        landed(in_bottom.at[dz], "bottom", dz)
        bottom[dz, 1] = add(bottom[dz, 1], in_bottom[dz, 1]).astype(bf16)
        push(bottom.at[dz, 1], last_bottom.at[dz], ("last_bottom", dz), e, tx)

    def third(dz):
        landed(last_top.at[dz], "last_top", dz)
        landed(last_bottom.at[dz], "last_bottom", dz)
        upper = add(top[dz, 0], in_top[dz, 0], last_top[dz])
        lower = add(bottom[dz, 0], in_bottom[dz, 0], last_bottom[dz])
        if dz:
            share[dz - 1, :half] = upper.astype(bf16)
            share[dz - 1, half:] = lower.astype(bf16)
            copy = pltpu.make_async_remote_copy(
                src_ref=share.at[dz - 1], dst_ref=arrived.at[z], send_sem=sent.at[len(started)],
                recv_sem=got.at[22 * nz + z], device_id={"ep": back(dz) * 2 + c, "tp": t},
                device_id_type=pl.DeviceIdType.MESH)
            copy.start()
            started.append(copy)
        return upper, lower

    def by_width(out, ref, dst):
        right = ref[...].reshape(ep * rows, ref.shape[2])
        for q in range(tp):
            out[pl.ds(q * cols, cols), :] = tn(full[:, 0, q].reshape(ep * rows, cols), right)
        bring(out, dst.at[0])

    spread(1)
    compute(0)
    if nz > 2:
        spread(2)
    for dz in range(1, nz):
        relay(dz)
        if dz + 2 < nz:
            spread(dz + 2)
        if dz > 1:
            second(dz - 2)
        first(dz - 1)
        hand(dz)
        compute(dz)
    for k in range(1, tp):
        push(score, scores.at[t], ("score", k), e, lax.rem(t + k, tp))
    scores[t] = score[...]
    for dz in range(1, nz - 2):
        third(dz)
    second(nz - 2)
    first(nz - 1)
    by_width(g_gate, d_gate, out_gate)
    for dz in range(max(1, nz - 2), nz - 1):
        third(dz)
    second(nz - 1)
    for k in range(1, tp):
        landed(scores.at[lax.rem(t - k + tp, tp)], "score", k)
    total[...] = add(*[scores[j] for j in range(tp)])
    for k in range(1, ep):
        to = lax.rem(e + k, ep)
        push(total.at[to], home.at[e], ("home", k), to, t)
    home[e] = total[e]
    by_width(g_up, d_up, out_up)
    third(nz - 1)
    left = act_w[...].reshape(ep * rows, act_w.shape[2])
    for q in range(tp):
        g_down[:, pl.ds(q * cols, cols)] = tn(left, full[:, 1, q].reshape(ep * rows, cols))
    bring(g_down, out_down.at[0])
    upper, lower = third(0)
    for k in range(1, nz):
        j = lax.rem(z + k, nz)
        pltpu.make_async_remote_copy(
            src_ref=arrived.at[j], dst_ref=arrived.at[j], send_sem=sent.at[0],
            recv_sem=got.at[22 * nz + j], device_id={"ep": side, "tp": t},
            device_id_type=pl.DeviceIdType.MESH).wait_recv()
        upper = upper + arrived[j, :half].astype(f32)
        lower = lower + arrived[j, half:].astype(f32)
    result[:half] = upper.astype(bf16)
    result[half:] = lower.astype(bf16)
    bring(result, out_tok)
    for k in range(1, ep):
        landed(home.at[lax.rem(e - k + ep, ep)], "home", k)
    for j in range(ep):
        out_home[pl.ds(j, 1), :] = home[j, :1]
    assert len(started) <= 20 * nz and len(slots) <= 20 * nz and len(relays) <= 4 * nz
    for copy in started:
        copy.wait_send()
    for go, copy in relays:
        pl.when(go)(copy.wait_send)
    for copy in locals_[len(own) + len(loads):]:
        copy.wait()


def dense(tokens, cotangent, routes, route_weight, w_gate, w_up, w_down):
    f32, bf16 = jnp.float32, jnp.bfloat16
    rows, width = tokens.shape
    ep, tp = lax.axis_size("ep"), lax.axis_size("tp")
    cols, half, nz, hidden = width // tp, rows // 2, ep // 2, w_gate.shape[2]
    hit = routes[None] == jnp.arange(ep, dtype=routes.dtype)[:, None, None]
    table = jnp.sum(jnp.where(hit, route_weight[None], 0.0), axis=2)
    anywhere, near = pl.BlockSpec(memory_space=pltpu.HBM), pl.BlockSpec(memory_space=pltpu.VMEM)
    shape = jax.ShapeDtypeStruct
    grad_tokens, home, gg, gu, gd = pl.pallas_call(
        functools.partial(kernel, ep, tp),
        out_shape=(shape((rows, cols), bf16), shape((ep, rows), f32), shape(w_gate.shape, f32),
                   shape(w_up.shape, f32), shape(w_down.shape, f32)),
        in_specs=[anywhere, anywhere, near, anywhere, anywhere, anywhere],
        out_specs=(anywhere, near, anywhere, anywhere, anywhere),
        scratch_shapes=[
            pltpu.VMEM((ep, 2, tp, rows, cols), bf16),
            pltpu.VMEM((width, hidden), bf16),
            pltpu.VMEM((width, hidden), bf16),
            pltpu.VMEM((hidden, width), bf16),
            pltpu.VMEM((ep, ep, rows), f32),
            pltpu.VMEM((ep, tp, rows, cols), bf16),
            pltpu.VMEM((nz, tp, rows, cols), bf16),
            pltpu.VMEM((nz, 4, half, cols), bf16),
            pltpu.VMEM((nz, 4, half, cols), bf16),
            pltpu.VMEM((nz, 2, half, cols), bf16),
            pltpu.VMEM((nz, 2, half, cols), bf16),
            pltpu.VMEM((nz, half, cols), bf16),
            pltpu.VMEM((nz, half, cols), bf16),
            pltpu.VMEM((nz - 1, rows, cols), bf16),
            pltpu.VMEM((nz, rows, cols), bf16),
            pltpu.VMEM((ep, rows, hidden), bf16),
            pltpu.VMEM((ep, rows, hidden), bf16),
            pltpu.VMEM((ep, rows, hidden), bf16),
            pltpu.VMEM((width, hidden), f32),
            pltpu.VMEM((width, hidden), f32),
            pltpu.VMEM((hidden, width), f32),
            pltpu.VMEM((ep, 8, rows), f32),
            pltpu.VMEM((tp, ep, 8, rows), f32),
            pltpu.VMEM((ep, 8, rows), f32),
            pltpu.VMEM((ep, 8, rows), f32),
            pltpu.VMEM((rows, cols), bf16),
            pltpu.SemaphoreType.DMA((16 + 2 * tp,)),
            pltpu.SemaphoreType.DMA((24 * nz,)),
            pltpu.SemaphoreType.DMA((24 * nz,)),
        ],
        compiler_params=pltpu.CompilerParams(
            collective_id=0, has_side_effects=True, vmem_limit_bytes=50 * 1024 * 1024),
    )(tokens, cotangent, table, w_gate, w_up, w_down)
    grw = jnp.sum(jnp.where(hit, home[:, :, None], 0.0), axis=0)
    return grad_tokens, grw, gg, gu, gd


def on_device(*args):
    rows, width = args[0].shape
    ep, tp = lax.axis_size("ep"), lax.axis_size("tp")
    fits = tp == 4 and ep % 2 == 0 and rows % 128 == 0 and 4 * rows * width * ep <= 1 << 24
    return (dense if fits else slotted)(*args)


def solution(mesh):
    return jax.shard_map(
        on_device,
        mesh=mesh,
        in_specs=(
            P("ep", None),
            P("ep", None),
            P("ep", None),
            P("ep", None),
            P("ep", None, "tp"),
            P("ep", None, "tp"),
            P("ep", "tp", None),
        ),
        out_specs=(
            P("ep", "tp"),
            P("ep", None),
            P("ep", None, "tp"),
            P("ep", None, "tp"),
            P("ep", "tp", None),
        ),
        check_vma=False,
    )
```
